256 devices in a mesh: sp: 32 (over z, y), tp: 8 (over x, core).
Axes of the slice: x: 4, y: 4, z: 8, core: 2. Of those that a mesh axis runs over, the one named last changes fastest.
Arguments:
- mix_input: bfloat16 [8192, 1024], P('sp', 'tp'), may hold values from -6 to 6
- stream: bfloat16 [8192, 2048], P(('sp', 'tp')), may hold values from -48 to 48
- doc_ids: int32 [8192], P('sp'), may hold values from 0 to 3, never falling along the last dimension, each value on 1 to 4096 neighbouring positions
- log_dt: float32 [64], P('tp'), may hold values from -12 to -2
- decay_rate: float32 [64, 64], P('tp'), may hold values from 0.5 to 1
- frequency: float32 [64, 64], P('tp'), may hold values from 0 to 64
- input_real: float32 [2, 64, 64, 16], P(None, 'tp'), may hold values from -400 to 400
- input_imag: float32 [2, 64, 64, 16], P(None, 'tp'), may hold values from -400 to 400
- output_real: float32 [2, 64, 16, 64], P(None, 'tp'), may hold values from -0.75 to 0.75
- output_imag: float32 [2, 64, 16, 64], P(None, 'tp'), may hold values from -0.75 to 0.75
- skip_gain: float32 [1024], P('tp'), may hold values from -4 to 4
- log_keep: float32 [64, 8192], P('tp', 'sp'), may hold values from -2 to 0
- proj_weight: bfloat16 [1024, 2048], P('tp'), may hold values from -0.1875 to 0.1875
- norm_gain: float32 [2048], replicated, may hold values from 0.1 to 1.9
- gate_weight: bfloat16 [2048, 5632], P('sp', 'tp'), may hold values from -0.125 to 0.125
- up_weight: bfloat16 [2048, 5632], P('sp', 'tp'), may hold values from -0.125 to 0.125
- down_weight: bfloat16 [5632, 2048], P('tp', 'sp'), may hold values from -0.078125 to 0.078125
Outputs:
- layer_out: bfloat16 [8192, 2048], P(('sp', 'tp'))
The draws below stay inside these ranges and needn't reach their ends.
Inputs may be any that keep to these rules, and one draw needn't show every extreme that they name: `doc_ids`: document numbers never fall along the positions; a document covers at most half of the positions.
All inputs are finite; a program needn't handle non-finite values.
Results may differ from the reference program's by a relative error of at most 0.009.
Values may be sent and summed in bfloat16 or wider, within the bound.
No kernel may reach another device: no remote copies, remote signals or barrier semaphores. Data moves between devices by JAX's collectives and lax.ppermute only.
A program may use at most 128 MiB of HBM per device.

```python
import math
import jax
import jax.numpy as jnp
import numpy as np
from jax import lax

D = 2048
WIDTH = 1024
GROUP = 16
STATE = 64
FF = 5632
TOK_DEV = 256
DOCS = 4
GROUPS = 64
TOKENS = 8192
N_TP = 8


def group_steps(key):
    base = jax.random.fold_in(key, 11)
    first_key, second_key, third_key = jax.random.split(base, 3)
    picked = jax.random.uniform(first_key, (GROUPS,), jnp.float32)
    slower = picked < 0.5
    slow_value = math.log(0.5 / TOKENS) + jax.random.uniform(second_key, (GROUPS,), jnp.float32, -0.3, 0.3)
    fast_value = jax.random.uniform(third_key, (GROUPS,), jnp.float32, math.log(0.04), math.log(0.05))
    return jnp.where(slower, slow_value, fast_value)


def draw_log_dt(key, part):
    return group_steps(key).astype(jnp.float32)


def input_matrix(key, salt):
    log_step = group_steps(key)
    scale = jnp.sqrt(2.0 / (jnp.exp(log_step) * GROUP))
    noise = jax.random.truncated_normal(jax.random.fold_in(key, salt), -4.0, 4.0, (2, GROUPS, STATE, GROUP), jnp.float32)
    return (noise * scale[None, :, None, None]).astype(jnp.float32)


def draw_input_real(key, part):
    return input_matrix(key, 21)


def draw_input_imag(key, part):
    return input_matrix(key, 22)


def draw_log_keep(key, part):
    base = jax.random.fold_in(key, 31)
    first_key, second_key, third_key, fourth_random_key = jax.random.split(base, 4)
    blocks = TOKENS // TOK_DEV
    level = jnp.exp(jax.random.uniform(first_key, (GROUPS, blocks), jnp.float32, math.log(0.1), 0.0)) / TOKENS
    per_slot_feedforward = jnp.repeat(level, TOK_DEV, axis=1) * jax.random.uniform(second_key, (GROUPS, TOKENS), jnp.float32, 0.0, 2.0)
    slot_indices = jax.random.randint(third_key, (GROUPS, 2), 0, TOKENS)
    stack_level_count = jax.random.uniform(fourth_random_key, (GROUPS, 2), jnp.float32, 0.22, 0.69)
    sequence_offsets = jnp.arange(TOKENS, dtype=jnp.int32)
    segment_sets = jnp.sum((sequence_offsets[None, None, :] == slot_indices[:, :, None]).astype(jnp.float32) * stack_level_count[:, :, None], axis=1)
    return (-(per_slot_feedforward + segment_sets)).astype(jnp.float32)


def draw_stream(key, part):
    base = jax.random.fold_in(key, 41)
    first_key, second_key, third_key = jax.random.split(base, 3)
    row_scale = jnp.exp(jax.random.uniform(first_key, (TOKENS, 1), jnp.float32, math.log(0.3), math.log(3.0)))
    col_scale = jnp.exp(jax.random.uniform(second_key, (1, D), jnp.float32, math.log(0.3), math.log(3.0)))
    values = jax.random.truncated_normal(third_key, -4.0, 4.0, (TOKENS, D), jnp.float32)
    return (values * row_scale * col_scale).astype(jnp.bfloat16)


def block_levels(own_key, extent, shards, least, largest):
    level = 1.0
    for axis_at, parts in shards:
        draws = jax.random.uniform(jax.random.fold_in(jax.random.fold_in(own_key, 6), axis_at), (parts,), jnp.float32, least / len(shards), largest / len(shards))
        level = level * jnp.repeat(jnp.exp(draws), extent[axis_at] // parts).reshape((-1,) + (1,) * (len(extent) - 1 - axis_at))
    return level


def split_up(amount, total, reach, slope):
    loads = [(1 << 20) // math.isqrt(rank ** slope) + 1 for rank in range(2, amount + 1)]
    surplus, holding = total - reach - (amount - 1), [1] * (amount - 1)
    while surplus > 0:
        candidates = [i for i in range(amount - 1) if holding[i] < reach]
        mass, left = sum([loads[i] for i in candidates]), surplus
        for i in candidates:
            extra = min(reach - holding[i], max(1, left * loads[i] // mass), surplus)
            holding[i] = holding[i] + extra
            surplus = surplus - extra
    return np.array([reach] + holding)


def uneven(rng, count, total, most, lean):
    if count == 2:
        one = jax.random.randint(rng, (), max(1, total - most), min(most, total - 1) + 1)
        return jnp.stack([one, total - one])
    sizes = jnp.asarray(split_up(count, total, most, lean), jnp.int32)
    couples = (count - 1) // 2
    giver, receiver = sizes[1:1 + 2 * couples:2], sizes[2:2 + 2 * couples:2]
    room = jnp.minimum(giver - 1, most - receiver)
    moved = jax.random.randint(jax.random.fold_in(rng, 1), (couples,), 0, 1 << 20) % (room + 1)
    sizes = sizes.at[1:1 + 2 * couples:2].set(giver - moved).at[2:2 + 2 * couples:2].set(receiver + moved)
    return sizes[jax.random.permutation(jax.random.fold_in(rng, 2), count)]


def scatter_about(stream_key, shape, scale, bound, cuts=(), kind=jnp.bfloat16):
    array = scale * jax.random.normal(stream_key, shape, jnp.float32)
    if cuts:
        array = array * block_levels(stream_key, shape, cuts, -0.22, 0.18)
    return jnp.clip(array, -bound, bound).astype(kind)


def setup_inputs(seed: int = 0) -> dict:
    streams_of = jax.random.split(jax.random.key(seed), 18)
    return {
        "mix_input": scatter_about(streams_of[0], (TOKENS, WIDTH), 1.0, 6.0, ((0, 32), (1, 8))),
        "stream": draw_stream(jax.random.fold_in(streams_of[17], 71), 0),
        "doc_ids": jnp.searchsorted(jnp.cumsum(uneven(streams_of[2], DOCS, TOKENS, TOKENS // 2, 0)), jnp.arange(TOKENS), side="right").astype(jnp.int32),
        "log_dt": draw_log_dt(jax.random.fold_in(streams_of[17], 71), 0),
        "decay_rate": jnp.clip(jnp.exp(math.log(1.0) - 0.6931472 * jax.random.uniform(streams_of[4], (GROUPS, STATE), jnp.float32) ** block_levels(streams_of[4], (GROUPS, STATE), ((0, 8),), -0.2, 0.2)), 0.5, 1.0),
        "frequency": jnp.clip(64.0 * jax.random.uniform(streams_of[5], (GROUPS, STATE), jnp.float32) ** block_levels(streams_of[5], (GROUPS, STATE), ((0, 8),), -0.2, 0.2), 0.0, 64.0),
        "input_real": draw_input_real(jax.random.fold_in(streams_of[17], 71), 0),
        "input_imag": draw_input_imag(jax.random.fold_in(streams_of[17], 71), 0),
        "output_real": scatter_about(streams_of[8], (2, GROUPS, GROUP, STATE), STATE ** -0.5, 0.75, ((1, 8),), jnp.float32),
        "output_imag": scatter_about(streams_of[9], (2, GROUPS, GROUP, STATE), STATE ** -0.5, 0.75, ((1, 8),), jnp.float32),
        "skip_gain": scatter_about(streams_of[10], (WIDTH,), 1.0, 4.0, ((0, 8),), jnp.float32),
        "log_keep": draw_log_keep(jax.random.fold_in(streams_of[17], 71), 0),
        "proj_weight": scatter_about(streams_of[12], (WIDTH, D), WIDTH ** -0.5, 0.1875, ((0, 8),)),
        "norm_gain": jnp.clip(1.0 + 0.18 * jax.random.normal(streams_of[13], (D,), jnp.float32), 0.1, 1.9),
        "gate_weight": scatter_about(streams_of[14], (D, FF), D ** -0.5, 0.125, ((0, 32), (1, 8))),
        "up_weight": scatter_about(streams_of[15], (D, FF), D ** -0.5, 0.125, ((0, 32), (1, 8))),
        "down_weight": scatter_about(streams_of[16], (FF, D), FF ** -0.5, 0.078125, ((0, 8), (1, 32))),
    }


HIGHEST = lax.Precision.HIGHEST

def discretize(log_dt, decay_rate, frequency):
    step_size = jnp.exp(log_dt)[:, None]
    magnitude = jnp.exp(-step_size * decay_rate)
    angle_step = step_size * frequency
    state_real = magnitude * jnp.cos(angle_step)
    state_imag = magnitude * jnp.sin(angle_step)
    denominator = decay_rate * decay_rate + frequency * frequency
    shifted = state_real - 1.0
    zoh_real = (-shifted * decay_rate + state_imag * frequency) / denominator
    holdfixed_angle_part = (-state_imag * decay_rate - shifted * frequency) / denominator
    return (state_real, state_imag, zoh_real, holdfixed_angle_part)

def input_maps(zoh_real, holdfixed_angle_part, input_real, input_imag):
    scale_real = zoh_real[None, :, :, None]
    scale_imag = holdfixed_angle_part[None, :, :, None]
    return (scale_real * input_real - scale_imag * input_imag, scale_real * input_imag + scale_imag * input_real)

def pair_combine(earlier, later):
    mult_one_real, mult_one_imag, first_state_real, state_one_imag = earlier
    mult_two_real, second_multiplier_imag, state_two_real, state_two_imag = later
    return (mult_two_real * mult_one_real - second_multiplier_imag * mult_one_imag, mult_two_real * mult_one_imag + second_multiplier_imag * mult_one_real, mult_two_real * first_state_real - second_multiplier_imag * state_one_imag + state_two_real, mult_two_real * state_one_imag + second_multiplier_imag * first_state_real + state_two_imag)

def rounded_sum(activations, weights, pieces):
    block_width = activations.shape[1] // pieces
    summed = jnp.zeros((activations.shape[0], weights.shape[1]), jnp.float32)
    for number in range(pieces):
        lower = number * block_width
        partial_value = jnp.dot(activations[:, lower:lower + block_width], weights[lower:lower + block_width], preferred_element_type=jnp.float32).astype(jnp.bfloat16)
        summed = summed + lax.optimization_barrier(partial_value).astype(jnp.float32)
    return summed

def reference(mix_input, stream, doc_ids, log_dt, decay_rate, frequency, input_real, input_imag, output_real, output_imag, skip_gain, log_keep, proj_weight, norm_gain, gate_weight, up_weight, down_weight):
    state_real, state_imag, zoh_real, holdfixed_angle_part = discretize(log_dt, decay_rate, frequency)
    map_real, map_imag = input_maps(zoh_real, holdfixed_angle_part, input_real, input_imag)
    channels = mix_input.astype(jnp.float32)
    grouped = channels.reshape(TOKENS, GROUPS, GROUP).transpose(1, 0, 2)
    same_doc = (doc_ids[1:] == doc_ids[:-1]).astype(jnp.float32)
    nothing = jnp.zeros((1,), jnp.float32)
    link_prev = jnp.concatenate([nothing, same_doc])
    link_next = jnp.concatenate([same_doc, nothing])
    keep_rates = jnp.exp(log_keep)

    def group_pass(packed):
        cluster_source, group_real, group_imag, group_map_real, group_map_imag, read_real, read_imag, keep_row = packed
        result = jnp.zeros((TOKENS, GROUP), jnp.float32)
        for direction, doc_links, reverse in ((0, link_prev, False), (1, link_next, True)):
            factor = (keep_row * doc_links)[:, None]
            mult_real = factor * group_real[None, :]
            mult_imag = factor * group_imag[None, :]
            drive_real = jnp.dot(cluster_source, group_map_real[direction].T, precision=HIGHEST)
            drive_imag = jnp.dot(cluster_source, group_map_imag[direction].T, precision=HIGHEST)
            scanned = lax.associative_scan(pair_combine, (mult_real, mult_imag, drive_real, drive_imag), reverse=reverse, axis=0)
            result = result + jnp.dot(scanned[2], read_real[direction].T, precision=HIGHEST)
            result = result - jnp.dot(scanned[3], read_imag[direction].T, precision=HIGHEST)
        return result
    outputs = lax.map(group_pass, (grouped, state_real, state_imag, map_real.transpose(1, 0, 2, 3), map_imag.transpose(1, 0, 2, 3), output_real.transpose(1, 0, 2, 3), output_imag.transpose(1, 0, 2, 3), keep_rates))
    mixed_pre = outputs.transpose(1, 0, 2).reshape(TOKENS, WIDTH) + skip_gain * channels
    mixed = jax.nn.gelu(mixed_pre).astype(jnp.bfloat16)
    branch = rounded_sum(mixed, proj_weight, N_TP)
    resid = stream.astype(jnp.float32) + branch
    scale = lax.rsqrt(lax.optimization_barrier(jnp.mean(resid * resid, axis=-1, keepdims=True)) + 1e-06)
    normed = (resid * scale * norm_gain).astype(jnp.bfloat16)
    block_width = FF // N_TP
    ffn = jnp.zeros((TOKENS, D), jnp.float32)
    for number in range(N_TP):
        lower = number * block_width
        gate = jnp.dot(normed, gate_weight[:, lower:lower + block_width], preferred_element_type=jnp.float32)
        upward = jnp.dot(normed, up_weight[:, lower:lower + block_width], preferred_element_type=jnp.float32)
        hidden = (jax.nn.silu(gate) * upward).astype(jnp.bfloat16)
        partial_value = jnp.dot(hidden, down_weight[lower:lower + block_width], preferred_element_type=jnp.float32).astype(jnp.bfloat16)
        ffn = ffn + lax.optimization_barrier(partial_value).astype(jnp.float32)
    return (resid + 0.5 * ffn).astype(jnp.bfloat16)
```

```python
import jax
import jax.numpy as jnp
from jax import lax
from jax.experimental import pallas as pl
from jax.experimental.pallas import tpu as pltpu
from jax.sharding import Mesh
from jax.sharding import PartitionSpec as P

GROUP = 16
SP = ("z", "y")
TP = ("x", "c")
HIGHEST = lax.Precision.HIGHEST


def discretize(log_dt, decay_rate, frequency):
    step_size = jnp.exp(log_dt)[:, None]
    magnitude = jnp.exp(-step_size * decay_rate)
    angle_step = step_size * frequency
    state_real = magnitude * jnp.cos(angle_step)
    state_imag = magnitude * jnp.sin(angle_step)
    denominator = decay_rate * decay_rate + frequency * frequency
    shifted = state_real - 1.0
    zoh_real = (-shifted * decay_rate + state_imag * frequency) / denominator
    zoh_imag = (-state_imag * decay_rate - shifted * frequency) / denominator
    return (state_real, state_imag, zoh_real, zoh_imag)


def input_maps(zoh_real, zoh_imag, input_real, input_imag):
    scale_real = zoh_real[None, :, :, None]
    scale_imag = zoh_imag[None, :, :, None]
    return (
        scale_real * input_real - scale_imag * input_imag,
        scale_real * input_imag + scale_imag * input_real,
    )


def on_ring(array, axis, shift):
    size = lax.axis_size(axis)
    return lax.ppermute(array, axis, [(i, (i + shift) % size) for i in range(size)])


def drive_matrix(map_real, map_imag):
    groups, states = map_real.shape[1:3]
    own = jnp.eye(groups, dtype=jnp.float32)[:, None, :, None]

    def spread(part):
        return (part[:, :, None, :] * own).reshape(groups, states, groups * GROUP)

    none = jnp.zeros((groups, states, groups * GROUP), jnp.float32)
    rows = []
    for part in (map_real, map_imag):
        rows.append(jnp.concatenate([spread(part[0]), none], axis=2))
        rows.append(jnp.concatenate([none, spread(part[1])], axis=2))
    return jnp.concatenate(rows, axis=1)


def read_matrix(read_real, read_imag):
    groups, width, states = read_real.shape[1:]
    own = jnp.eye(groups, dtype=jnp.float32)[:, :, None, None]
    none = jnp.zeros((groups, width, states), jnp.float32)

    def spread(part):
        return (part[:, None] * own).reshape(groups, groups * width, 4 * states)

    ahead = jnp.concatenate([read_real[0], none, -read_imag[0], none], axis=2)
    back = jnp.concatenate([none, read_real[1], none, -read_imag[1]], axis=2)
    return jnp.concatenate([spread(ahead), spread(back)], axis=1)


def flip_matrix(count, dtype):
    rows = lax.broadcasted_iota(jnp.int32, (count, count), 0)
    cols = lax.broadcasted_iota(jnp.int32, (count, count), 1)
    return jnp.where(rows + cols == count - 1, 1.0, 0.0).astype(dtype)


def times_transposed(left, right, precision=None):
    return lax.dot_general(
        left,
        right,
        (((1,), (1,)), ((), ())),
        precision=precision,
        preferred_element_type=jnp.float32,
    )


def local_states_kernel(
    u_ref, factor_ref, drive_ref, pole_ref, docs_ref, real_ref, imag_ref, decay_ref, summary_ref
):
    tokens, channels = u_ref.shape
    groups, lanes = pole_ref.shape[1:]
    u = u_ref[...]
    backward = jnp.dot(
        flip_matrix(tokens, jnp.bfloat16), u, preferred_element_type=jnp.float32
    ).astype(jnp.bfloat16)
    both = jnp.concatenate([u, backward], axis=1)
    ahead = lax.broadcasted_iota(jnp.int32, (tokens, lanes), 1) < lanes // 2
    for g in range(groups):
        whole = drive_ref[g]
        first = whole.astype(jnp.bfloat16)
        rest = whole - first.astype(jnp.float32)
        second = rest.astype(jnp.bfloat16)
        third = (rest - second.astype(jnp.float32)).astype(jnp.bfloat16)
        drive = times_transposed(both, first)
        drive = drive + times_transposed(both, second)
        drive = drive + times_transposed(both, third)
        real_ref[:, g, :] = drive[:, :lanes]
        imag_ref[:, g, :] = drive[:, lanes:]
        decay_ref[:, g, :] = jnp.where(
            ahead, factor_ref[:, g : g + 1], factor_ref[:, groups + g : groups + g + 1]
        )
    pole_real, pole_imag = (pole_ref[0], pole_ref[1])

    def step(t, carry):
        state_real, state_imag, product = carry
        factor = decay_ref[t]
        step_real, step_imag = (factor * pole_real, factor * pole_imag)
        return (
            step_real * state_real - step_imag * state_imag + real_ref[t],
            step_real * state_imag + step_imag * state_real + imag_ref[t],
            product * factor,
        )

    zero = jnp.zeros((groups, lanes), jnp.float32)
    state_real, state_imag, product = lax.fori_loop(
        0, tokens, step, (zero, zero, zero + 1.0), unroll=8
    )
    summary_ref[0] = state_real
    summary_ref[1] = state_imag
    summary_ref[2] = product
    summary_ref[3] = docs_ref[...]


def mixing_kernel(
    place_ref,
    all_ref,
    u_ref,
    real_ref,
    imag_ref,
    decay_ref,
    pole_ref,
    docs_ref,
    read_ref,
    skip_ref,
    out_ref,
    state_real_ref,
    state_imag_ref,
    mixed_ref,
):
    tokens, channels = u_ref.shape
    groups, lanes = pole_ref.shape[1:]
    blocks = all_ref.shape[0]
    here = place_ref[0]
    pole_real, pole_imag = (pole_ref[0], pole_ref[1])
    far_real, far_imag = (pole_real, pole_imag)
    for _ in range(tokens.bit_length() - 1):
        far_real, far_imag = (far_real * far_real - far_imag * far_imag, 2.0 * far_real * far_imag)
    ahead = lax.broadcasted_iota(jnp.int32, (groups, lanes), 1) < lanes // 2

    def near_of(code):
        return jnp.floor(code * 0.125)

    def join(j, carry):
        state_real, state_imag, last = carry
        other = blocks - 1 - j
        local_real, local_imag, product, code = (
            jnp.where(ahead, all_ref[j, k], all_ref[other, k]) for k in range(4)
        )
        before = jnp.where(ahead, jnp.where(j < here, 1, 0), jnp.where(other > here, 1, 0)) > 0
        near = near_of(code)
        kept = jnp.where(near == last, product, 0.0)
        next_real = kept * (far_real * state_real - far_imag * state_imag) + local_real
        next_imag = kept * (far_real * state_imag + far_imag * state_real) + local_imag
        return (
            jnp.where(before, next_real, state_real),
            jnp.where(before, next_imag, state_imag),
            jnp.where(before, code - 8.0 * near, last),
        )

    zero = jnp.zeros((groups, lanes), jnp.float32)
    enter_real, enter_imag, last = lax.fori_loop(0, blocks - 1, join, (zero, zero, zero - 1.0))
    joined = near_of(docs_ref[...]) == last
    enter_real = jnp.where(joined, enter_real, 0.0)
    enter_imag = jnp.where(joined, enter_imag, 0.0)

    def step(t, carry):
        state_real, state_imag = carry
        factor = decay_ref[t]
        step_real, step_imag = (factor * pole_real, factor * pole_imag)
        next_real = step_real * state_real - step_imag * state_imag + real_ref[t]
        next_imag = step_real * state_imag + step_imag * state_real + imag_ref[t]
        state_real_ref[t] = next_real
        state_imag_ref[t] = next_imag
        return (next_real, next_imag)

    lax.fori_loop(0, tokens, step, (enter_real, enter_imag), unroll=8)
    read = jnp.zeros((tokens, 2 * channels), jnp.float32)
    for g in range(groups):
        states = jnp.concatenate([state_real_ref[:, g, :], state_imag_ref[:, g, :]], axis=1)
        read = read + times_transposed(states, read_ref[g], HIGHEST)
    backward = jnp.dot(
        flip_matrix(tokens, jnp.float32),
        read[:, channels:],
        precision=HIGHEST,
        preferred_element_type=jnp.float32,
    )
    pre = read[:, :channels] + backward + skip_ref[...] * u_ref[...].astype(jnp.float32)
    mixed_ref[...] = jax.nn.gelu(pre)
    rows = tokens // 8
    for k in range(8):
        start = pl.multiple_of(place_ref[1 + k] * rows, rows)
        out_ref[k * rows : (k + 1) * rows, :] = mixed_ref[pl.ds(start, rows), :].astype(
            jnp.bfloat16
        )


def feed_forward_kernel(
    rows_ref, gate_ref, up_ref, down_ref, keep_ref, send_ref, gate_acc, up_acc, hidden_ref
):
    i = pl.program_id(0)
    half = pl.num_programs(0) // 2
    shards, depth, hidden = gate_ref.shape

    @pl.when(i == 0)
    def _():
        gate_acc[...] = jnp.zeros(gate_acc.shape, jnp.float32)
        up_acc[...] = jnp.zeros(up_acc.shape, jnp.float32)

    @pl.when(i < half)
    def _():
        rows = rows_ref[...]
        gate_acc[...] += jnp.dot(
            rows,
            gate_ref[...].reshape(shards * depth, hidden),
            preferred_element_type=jnp.float32,
        )
        up_acc[...] += jnp.dot(
            rows, up_ref[...].reshape(shards * depth, hidden), preferred_element_type=jnp.float32
        )

    @pl.when(i == half - 1)
    def _():
        gate = gate_acc[...]
        hidden_ref[...] = (gate / (1.0 + jnp.exp(-gate)) * up_acc[...]).astype(jnp.bfloat16)

    @pl.when(i >= half)
    def _():
        made = times_transposed(
            hidden_ref[...], down_ref[...].reshape(shards * depth, hidden)
        )
        near = keep_ref.shape[0]
        keep_ref[...] = made[:near]
        send_ref[...] = made[near:].astype(jnp.bfloat16)


def feed_forward(rows, weights):
    tokens, features = rows.shape
    blocks, depth, hidden = weights.shape
    depth //= 3
    shards = 8
    half = blocks // shards
    width = shards * depth
    near = tokens // 2

    def weight_spec(which):
        if which < 2:
            return pl.BlockSpec(
                (shards, depth, hidden), lambda i: (jnp.minimum(i, half - 1), which, 0)
            )
        return pl.BlockSpec((shards, depth, hidden), lambda i: (jnp.maximum(i - half, 0), which, 0))

    return pl.pallas_call(
        feed_forward_kernel,
        grid=(2 * half,),
        in_specs=[
            pl.BlockSpec((tokens, width), lambda i: (0, jnp.minimum(i, half - 1))),
            weight_spec(0),
            weight_spec(1),
            weight_spec(2),
        ],
        out_specs=[
            pl.BlockSpec((near, width), lambda i: (0, jnp.maximum(i - half, 0))),
            pl.BlockSpec((near, width), lambda i: (0, jnp.maximum(i - half, 0))),
        ],
        out_shape=[
            jax.ShapeDtypeStruct((near, features), jnp.float32),
            jax.ShapeDtypeStruct((near, features), jnp.bfloat16),
        ],
        scratch_shapes=[
            pltpu.VMEM((tokens, hidden), jnp.float32),
            pltpu.VMEM((tokens, hidden), jnp.float32),
            pltpu.VMEM((tokens, hidden), jnp.bfloat16),
        ],
        name="feed_forward",
    )(rows, weights, weights, weights)


def summed_over_tp(keep, send):
    pair = keep + on_ring(send, "c", 1).astype(jnp.float32)
    chips = lax.axis_size("x")
    rows = pair.shape[0] // chips
    total = pair[:rows]
    away = pair.astype(jnp.bfloat16)
    for k in range(1, chips):
        arrived = on_ring(away[k * rows : (k + 1) * rows], "x", -k)
        total = total + arrived.astype(jnp.float32)
    return total


def rows_of_tp(array):
    chips = lax.axis_size("x")
    mine = jnp.concatenate([array] + [on_ring(array, "x", k) for k in range(1, chips)], axis=0)
    return jnp.concatenate([mine, on_ring(mine, "c", 1)], axis=0)


def local(
    mix_input,
    stream,
    doc_ids,
    log_dt,
    decay_rate,
    frequency,
    input_real,
    input_imag,
    output_real,
    output_imag,
    skip_gain,
    log_keep,
    proj_weight,
    norm_gain,
    gate_weight,
    up_weight,
    down_weight,
):
    weights = lax.all_gather(
        jnp.concatenate([gate_weight, up_weight, down_weight.T], axis=0), SP, axis=0, tiled=False
    )
    blocks = lax.axis_size(SP)
    chips = lax.axis_size("x")
    here, chip, core = (lax.axis_index(SP), lax.axis_index("x"), lax.axis_index("c"))
    tokens, channels = mix_input.shape
    groups, states = decay_rate.shape
    state_real, state_imag, zoh_real, zoh_imag = discretize(log_dt, decay_rate, frequency)
    map_real, map_imag = input_maps(zoh_real, zoh_imag, input_real, input_imag)
    drive = drive_matrix(map_real, map_imag)
    reader = read_matrix(output_real, output_imag)
    poles = jnp.stack([jnp.concatenate([part, part], axis=1) for part in (state_real, state_imag)])
    same_doc = (doc_ids[1:] == doc_ids[:-1]).astype(jnp.float32)
    single = jnp.ones((1,), jnp.float32)
    keep_rates = jnp.exp(log_keep)
    factors = jnp.concatenate(
        [
            (keep_rates * jnp.concatenate([single, same_doc])).T,
            (keep_rates * jnp.concatenate([same_doc, single])).T[::-1],
        ],
        axis=1,
    )
    first_doc, last_doc = (doc_ids[0].astype(jnp.float32), doc_ids[-1].astype(jnp.float32))
    ahead = lax.broadcasted_iota(jnp.int32, (groups, 2 * states), 1) < states
    docs = jnp.where(ahead, 8.0 * first_doc + last_doc, 8.0 * last_doc + first_doc)
    lanes = 2 * states
    by_token = jax.ShapeDtypeStruct((tokens, groups, lanes), jnp.float32)
    drive_real, drive_imag, decays, summary = pl.pallas_call(
        local_states_kernel,
        out_shape=[by_token] * 3 + [jax.ShapeDtypeStruct((4, groups, lanes), jnp.float32)],
        name="local_states",
    )(mix_input, factors, drive, poles, docs)
    everyone = lax.all_to_all(
        jnp.broadcast_to(summary, (blocks, *summary.shape)),
        SP,
        split_axis=0,
        concat_axis=0,
        tiled=True,
    )
    order = [
        2 * ((chip - k) % chips) + (core if own else 1 - core)
        for own in (True, False)
        for k in range(4)
    ]
    place = jnp.stack([here, *order]).astype(jnp.int32)
    vmem = pl.BlockSpec(memory_space=pltpu.VMEM)
    mixed = pl.pallas_call(
        mixing_kernel,
        out_shape=jax.ShapeDtypeStruct((tokens, channels), jnp.bfloat16),
        in_specs=[pl.BlockSpec(memory_space=pltpu.SMEM)] + [vmem] * 9,
        scratch_shapes=[
            pltpu.VMEM((tokens, groups, lanes), jnp.float32),
            pltpu.VMEM((tokens, groups, lanes), jnp.float32),
            pltpu.VMEM((tokens, channels), jnp.float32),
        ],
        name="mixing",
    )(
        place,
        everyone,
        mix_input,
        drive_real,
        drive_imag,
        decays,
        poles,
        docs,
        reader,
        skip_gain[None],
    )
    product = jnp.dot(mixed, proj_weight, preferred_element_type=jnp.float32)
    branch = summed_over_tp(product[: tokens // 2], product[tokens // 2 :].astype(jnp.bfloat16))
    resid = stream.astype(jnp.float32) + branch
    scale = lax.rsqrt(jnp.mean(resid * resid, axis=-1, keepdims=True) + 1e-06)
    normed = (resid * scale * norm_gain).astype(jnp.bfloat16)
    ffn = summed_over_tp(*feed_forward(rows_of_tp(normed), weights))
    return (resid + 0.5 * ffn).astype(jnp.bfloat16)


def solution(mesh):
    torus = Mesh(mesh.devices.reshape(8, 4, 4, 2), ("z", "y", "x", "c"))
    everything = SP + TP
    in_specs = (
        P(SP, TP),
        P(everything, None),
        P(SP),
        P(TP),
        P(TP, None),
        P(TP, None),
        P(None, TP, None, None),
        P(None, TP, None, None),
        P(None, TP, None, None),
        P(None, TP, None, None),
        P(TP),
        P(TP, SP),
        P(TP, None),
        P(),
        P(SP, TP),
        P(SP, TP),
        P(TP, SP),
    )
    return jax.shard_map(
        local, mesh=torus, in_specs=in_specs, out_specs=P(everything, None), check_vma=False
    )
```

```python
import jax
import jax.numpy as jnp
from jax import lax
from jax.experimental import pallas as pl
from jax.experimental.pallas import tpu as pltpu
from jax.sharding import Mesh
from jax.sharding import PartitionSpec as P


GROUP = 16
COST = 2_000_000_000
SP = ("z", "y")
TP = ("x", "c")
HIGHEST = lax.Precision.HIGHEST


def discretize(log_dt, decay_rate, frequency):
    step_size = jnp.exp(log_dt)
    magnitude = jnp.exp(-step_size * decay_rate)
    angle_step = step_size * frequency
    state_real = magnitude * jnp.cos(angle_step)
    state_imag = magnitude * jnp.sin(angle_step)
    denominator = decay_rate * decay_rate + frequency * frequency
    shifted = state_real - 1.0
    zoh_real = (-shifted * decay_rate + state_imag * frequency) / denominator
    zoh_imag = (-state_imag * decay_rate - shifted * frequency) / denominator
    return (state_real, state_imag, zoh_real, zoh_imag)


def on_ring(array, axis, shift):
    size = lax.axis_size(axis)
    return lax.ppermute(array, axis, [(i, (i + shift) % size) for i in range(size)])


def flip_matrix(count, dtype):
    rows = lax.broadcasted_iota(jnp.int32, (count, count), 0)
    cols = lax.broadcasted_iota(jnp.int32, (count, count), 1)
    return jnp.where(rows + cols == count - 1, 1.0, 0.0).astype(dtype)


def times_transposed(left, right, precision=None):
    return lax.dot_general(
        left,
        right,
        (((1,), (1,)), ((), ())),
        precision=precision,
        preferred_element_type=jnp.float32,
    )


def side_by_side(left, right):
    return jnp.concatenate([left, right], axis=1)


def local_states_kernel(
    u_ref,
    keep_ref,
    docs_ref,
    dt_ref,
    rates_ref,
    freq_ref,
    map_real_ref,
    map_imag_ref,
    real_ref,
    imag_ref,
    decay_ref,
    pole_ref,
    summary_ref,
    drive_ref,
):
    tokens, channels = u_ref.shape
    groups, lanes = pole_ref.shape[1:]
    diagonal = lax.broadcasted_iota(jnp.int32, (groups, groups), 0) == lax.broadcasted_iota(
        jnp.int32, (groups, groups), 1
    )
    log_dt = jnp.sum(jnp.where(diagonal, dt_ref[...], 0.0), axis=1, keepdims=True)
    state_real, state_imag, zoh_real, zoh_imag = discretize(
        log_dt, side_by_side(rates_ref[...], rates_ref[...]), side_by_side(freq_ref[...], freq_ref[...])
    )
    pole_ref[0] = state_real
    pole_ref[1] = state_imag
    docs = docs_ref[...].astype(jnp.float32)
    place = lax.broadcasted_iota(jnp.int32, docs.shape, 1)
    from_left = (docs == pltpu.roll(docs, 1, 1)) | (place == 0)
    from_right = (docs == pltpu.roll(docs, tokens - 1, 1)) | (place == tokens - 1)
    keep = jnp.exp(keep_ref[...])
    factors = jnp.concatenate(
        [jnp.where(from_left, keep, 0.0), jnp.where(from_right, keep, 0.0)], axis=0
    )
    flip = flip_matrix(tokens, jnp.float32)
    rows = lax.broadcasted_iota(jnp.int32, (tokens, tokens), 0)
    cols = lax.broadcasted_iota(jnp.int32, (tokens, tokens), 1)
    same = jnp.where(rows == cols, 1.0, 0.0)
    ahead_factor = times_transposed(same, factors, HIGHEST)
    back_factor = times_transposed(flip, factors, HIGHEST)
    u = u_ref[...]
    backward = jnp.dot(
        flip.astype(jnp.bfloat16), u, preferred_element_type=jnp.float32
    ).astype(jnp.bfloat16)
    both = jnp.concatenate([u, backward], axis=1)
    ahead = lax.broadcasted_iota(jnp.int32, (tokens, lanes), 1) < lanes // 2
    part = ahead[:GROUP]
    drive_ref[...] = jnp.zeros(drive_ref.shape, jnp.float32)
    for g in range(groups):
        scale_real, scale_imag = (zoh_real[g : g + 1], zoh_imag[g : g + 1])
        in_real, in_imag = (
            side_by_side(ref[0, g], ref[1, g]) for ref in (map_real_ref, map_imag_ref)
        )
        map_real = scale_real * in_real - scale_imag * in_imag
        map_imag = scale_real * in_imag + scale_imag * in_real
        at = g * GROUP
        drive_ref[at : at + GROUP, :lanes] = jnp.where(part, map_real, 0.0)
        drive_ref[at : at + GROUP, lanes:] = jnp.where(part, map_imag, 0.0)
        drive_ref[channels + at : channels + at + GROUP, :lanes] = jnp.where(part, 0.0, map_real)
        drive_ref[channels + at : channels + at + GROUP, lanes:] = jnp.where(part, 0.0, map_imag)
        whole = drive_ref[...]
        drive_ref[at : at + GROUP] = jnp.zeros((GROUP, 2 * lanes), jnp.float32)
        drive_ref[channels + at : channels + at + GROUP] = jnp.zeros(
            (GROUP, 2 * lanes), jnp.float32
        )
        first = whole.astype(jnp.bfloat16)
        rest = whole - first.astype(jnp.float32)
        second = rest.astype(jnp.bfloat16)
        third = (rest - second.astype(jnp.float32)).astype(jnp.bfloat16)
        drive = jnp.dot(both, first, preferred_element_type=jnp.float32)
        drive = drive + jnp.dot(both, second, preferred_element_type=jnp.float32)
        drive = drive + jnp.dot(both, third, preferred_element_type=jnp.float32)
        real_ref[:, g, :] = drive[:, :lanes]
        imag_ref[:, g, :] = drive[:, lanes:]
        decay_ref[:, g, :] = jnp.where(
            ahead, ahead_factor[:, g : g + 1], back_factor[:, groups + g : groups + g + 1]
        )
    pole_real, pole_imag = (pole_ref[0], pole_ref[1])

    def step(t, carry):
        state_real, state_imag, product = carry
        factor = decay_ref[t]
        step_real, step_imag = (factor * pole_real, factor * pole_imag)
        return (
            step_real * state_real - step_imag * state_imag + real_ref[t],
            step_real * state_imag + step_imag * state_real + imag_ref[t],
            product * factor,
        )

    zero = jnp.zeros((groups, lanes), jnp.float32)
    state_real, state_imag, product = lax.fori_loop(
        0, tokens, step, (zero, zero, zero + 1.0), unroll=8
    )
    summary_ref[0] = state_real
    summary_ref[1] = state_imag
    summary_ref[2] = product
    first_doc, last_doc = (
        jnp.broadcast_to(docs[:, :1], (groups, lanes)),
        jnp.broadcast_to(docs[:, tokens - 1 :], (groups, lanes)),
    )
    summary_ref[3] = jnp.where(
        ahead[:groups], 8.0 * first_doc + last_doc, 8.0 * last_doc + first_doc
    )


def near_of(code):
    return jnp.floor(code * 0.125)


def squared(real, imag, times):
    for _ in range(times):
        real, imag = (real * real - imag * imag, 2.0 * real * imag)
    return (real, imag)


def pick(ref, ahead, j, last):
    return tuple(jnp.where(ahead, ref[j, k], ref[last - j, k]) for k in range(4))


def row_kernel(place_ref, own_ref, *refs):
    arrived, pole_ref, row_ref, group_ref = (refs[:3], refs[3], refs[4], refs[5])
    groups, lanes = pole_ref.shape[1:]
    row_ref[place_ref[1]] = own_ref[...]
    for back, ref in zip((1, 3, 2), arrived):
        row_ref[(place_ref[1] + 4 - back) % 4] = ref[...]
    ahead = lax.broadcasted_iota(jnp.int32, (groups, lanes), 1) < lanes // 2
    far_real, far_imag = squared(pole_ref[0], pole_ref[1], 8)
    state_real, state_imag, product, code = pick(row_ref, ahead, 0, 3)
    first = near_of(code)
    last = code - 8.0 * first
    for j in range(1, 4):
        local_real, local_imag, factor, code = pick(row_ref, ahead, j, 3)
        near = near_of(code)
        kept = jnp.where(near == last, factor, 0.0)
        last = code - 8.0 * near
        state_real, state_imag = (
            kept * (far_real * state_real - far_imag * state_imag) + local_real,
            kept * (far_real * state_imag + far_imag * state_real) + local_imag,
        )
        product = product * kept
    group_ref[0] = state_real
    group_ref[1] = state_imag
    group_ref[2] = product
    group_ref[3] = 8.0 * first + last


def mixing_kernel(
    place_ref,
    row_ref,
    *refs,
):
    group_refs = refs[:8]
    (
        u_ref,
        real_ref,
        imag_ref,
        decay_ref,
        pole_ref,
        read_real_ref,
        read_imag_ref,
        skip_ref,
        out_ref,
        all_ref,
        state_real_ref,
        state_imag_ref,
        mixed_ref,
        matrix_ref,
    ) = refs[8:]
    tokens, channels = u_ref.shape
    groups, lanes = pole_ref.shape[1:]
    pole_real, pole_imag = (pole_ref[0], pole_ref[1])
    for back, ref in enumerate(group_refs):
        all_ref[(place_ref[0] + 8 - back) % 8] = ref[...]
    ahead = lax.broadcasted_iota(jnp.int32, (groups, lanes), 1) < lanes // 2
    zero = jnp.zeros((groups, lanes), jnp.float32)
    state = (zero, zero, zero - 1.0)
    for ref, here, blocks, far in (
        (all_ref, place_ref[0], 8, squared(pole_real, pole_imag, 10)),
        (row_ref, place_ref[1], 4, squared(pole_real, pole_imag, 8)),
    ):
        for j in range(blocks - 1):
            state_real, state_imag, last = state
            local_real, local_imag, product, code = pick(ref, ahead, j, blocks - 1)
            ours = jnp.where(j < here, 1, 0)
            theirs = jnp.where(blocks - 1 - j > here, 1, 0)
            before = jnp.where(ahead, ours, theirs) > 0
            near = near_of(code)
            kept = jnp.where(near == last, product, 0.0)
            next_real = kept * (far[0] * state_real - far[1] * state_imag) + local_real
            next_imag = kept * (far[0] * state_imag + far[1] * state_real) + local_imag
            state = (
                jnp.where(before, next_real, state_real),
                jnp.where(before, next_imag, state_imag),
                jnp.where(before, code - 8.0 * near, last),
            )
    joined = near_of(row_ref[place_ref[1], 3]) == state[2]
    enter_real = jnp.where(joined, state[0], 0.0)
    enter_imag = jnp.where(joined, state[1], 0.0)

    def step(t, carry):
        state_real, state_imag = carry
        factor = decay_ref[t]
        step_real, step_imag = (factor * pole_real, factor * pole_imag)
        next_real = step_real * state_real - step_imag * state_imag + real_ref[t]
        next_imag = step_real * state_imag + step_imag * state_real + imag_ref[t]
        state_real_ref[t] = next_real
        state_imag_ref[t] = next_imag
        return (next_real, next_imag)

    lax.fori_loop(0, tokens, step, (enter_real, enter_imag), unroll=8)
    read = jnp.zeros((tokens, 2 * channels), jnp.float32)
    matrix_ref[...] = jnp.zeros(matrix_ref.shape, jnp.float32)
    part = lax.broadcasted_iota(jnp.int32, (GROUP, lanes), 1) < lanes // 2
    for g in range(groups):
        states = jnp.concatenate([state_real_ref[:, g, :], state_imag_ref[:, g, :]], axis=1)
        out_real = side_by_side(read_real_ref[0, g], read_real_ref[1, g])
        out_imag = -side_by_side(read_imag_ref[0, g], read_imag_ref[1, g])
        at = g * GROUP
        matrix_ref[at : at + GROUP, :lanes] = jnp.where(part, out_real, 0.0)
        matrix_ref[at : at + GROUP, lanes:] = jnp.where(part, out_imag, 0.0)
        matrix_ref[channels + at : channels + at + GROUP, :lanes] = jnp.where(part, 0.0, out_real)
        matrix_ref[channels + at : channels + at + GROUP, lanes:] = jnp.where(part, 0.0, out_imag)
        read = read + times_transposed(states, matrix_ref[...], HIGHEST)
        matrix_ref[at : at + GROUP] = jnp.zeros((GROUP, 2 * lanes), jnp.float32)
        matrix_ref[channels + at : channels + at + GROUP] = jnp.zeros(
            (GROUP, 2 * lanes), jnp.float32
        )
    backward = jnp.dot(
        flip_matrix(tokens, jnp.float32),
        read[:, channels:],
        precision=HIGHEST,
        preferred_element_type=jnp.float32,
    )
    pre = read[:, :channels] + backward + skip_ref[...] * u_ref[...].astype(jnp.float32)
    mixed_ref[...] = jax.nn.gelu(pre)
    rows = tokens // 8
    for k in range(8):
        start = pl.multiple_of(place_ref[2 + k] * rows, rows)
        out_ref[k * rows : (k + 1) * rows, :] = mixed_ref[pl.ds(start, rows), :].astype(
            jnp.bfloat16
        )


def feed_forward_kernel(
    place_ref,
    rows_ref,
    own_ref,
    low_left_ref,
    high_left_ref,
    low_right_ref,
    high_right_ref,
    low_far_ref,
    high_far_ref,
    down_ref,
    keep_ref,
    send_ref,
    gate_to,
    up_to,
    down_to,
    sems,
):
    depth, hidden = down_to.shape[2:]
    half = low_far_ref.shape[0]
    column = [(place_ref[1] + 4 - back) % 4 for back in (0, 1, 3, 2)]
    copies = ([], [], [])
    for which, target in enumerate((gate_to, up_to)):
        span = pl.ds(which * depth, depth)
        for source, dest in (
            (own_ref, target.at[:, column[0]]),
            (low_left_ref, target.at[:half, column[1]]),
            (high_left_ref, target.at[half:, column[1]]),
            (low_right_ref, target.at[:half, column[2]]),
            (high_right_ref, target.at[half:, column[2]]),
            (low_far_ref, target.at[:half, column[3]]),
            (high_far_ref, target.at[half:, column[3]]),
        ):
            copies[which].append(pltpu.make_async_copy(source.at[:, span], dest, sems.at[which]))
    for m in range(4):
        copies[2].append(
            pltpu.make_async_copy(
                down_ref.at[:, pl.ds(m * depth, depth)], down_to.at[:, column[m]], sems.at[2]
            )
        )
    for group in copies:
        for copy in group:
            copy.start()
    rows = rows_ref[...]
    features = rows.shape[1]
    for copy in copies[0]:
        copy.wait()
    gate = jnp.dot(
        rows, gate_to[...].reshape(features, hidden), preferred_element_type=jnp.float32
    )
    for copy in copies[1]:
        copy.wait()
    up = jnp.dot(rows, up_to[...].reshape(features, hidden), preferred_element_type=jnp.float32)
    inner = (gate / (1.0 + jnp.exp(-gate)) * up).astype(jnp.bfloat16)
    for copy in copies[2]:
        copy.wait()
    near = keep_ref.shape[0]
    count = 2
    width = count * 4 * depth
    for z in range(0, down_to.shape[0], count):
        made = times_transposed(inner, down_to[z : z + count].reshape(width, hidden))
        at = z * 4 * depth
        keep_ref[:, at : at + width] = made[:near]
        send_ref[:, at : at + width] = made[near:].astype(jnp.bfloat16)


def feed_forward(place, rows, pieces):
    tokens, features = rows.shape
    hidden = pieces[0].shape[2]
    scratch = pltpu.VMEM((8, 4, features // 32, hidden), jnp.bfloat16)
    return pl.pallas_call(
        feed_forward_kernel,
        in_specs=[IN_SMEM, IN_VMEM] + [pl.BlockSpec(memory_space=pl.ANY)] * len(pieces),
        out_shape=[
            jax.ShapeDtypeStruct((tokens // 2, features), jnp.float32),
            jax.ShapeDtypeStruct((tokens // 2, features), jnp.bfloat16),
        ],
        scratch_shapes=[scratch, scratch, scratch, pltpu.SemaphoreType.DMA((3,))],
        name="feed_forward",
    )(place, rows, *pieces)


IN_VMEM = pl.BlockSpec(memory_space=pltpu.VMEM)
IN_SMEM = pl.BlockSpec(memory_space=pltpu.SMEM)


def summed_over_tp(keep, send):
    pair = keep + on_ring(send, "c", 1).astype(jnp.float32)
    chips = lax.axis_size("x")
    rows = pair.shape[0] // chips
    total = pair[:rows]
    away = pair.astype(jnp.bfloat16)
    for k in range(1, chips):
        arrived = on_ring(away[k * rows : (k + 1) * rows], "x", -k)
        total = total + arrived.astype(jnp.float32)
    return total


def local(
    mix_input,
    stream,
    doc_ids,
    log_dt,
    decay_rate,
    frequency,
    input_real,
    input_imag,
    output_real,
    output_imag,
    skip_gain,
    log_keep,
    proj_weight,
    norm_gain,
    gate_weight,
    up_weight,
    down_weight,
):
    chips = lax.axis_size("x")
    chip, core = (lax.axis_index("x"), lax.axis_index("c"))
    tokens, channels = mix_input.shape
    groups, states = decay_rate.shape
    lanes = 2 * states
    spare = -gate_weight.shape[1] % 128
    gate_up = jnp.pad(jnp.concatenate([gate_weight, up_weight], axis=0), ((0, 0), (0, spare)))
    own = lax.all_gather(gate_up, "z", axis=0, tiled=False)
    down = jnp.pad(down_weight.T, ((0, 0), (0, spare)))
    down_row = [on_ring(down, "y", k) for k in (1, -1, 2)]
    by_token = jax.ShapeDtypeStruct((tokens, groups, lanes), jnp.float32)
    drive_real, drive_imag, decays, poles, summary = pl.pallas_call(
        local_states_kernel,
        out_shape=[by_token] * 3
        + [jax.ShapeDtypeStruct((k, groups, lanes), jnp.float32) for k in (2, 4)],
        scratch_shapes=[pltpu.VMEM((2 * channels, 2 * lanes), jnp.float32)],
        name="local_states",
    )(
        mix_input,
        log_keep,
        doc_ids[None],
        log_dt[None],
        decay_rate,
        frequency,
        input_real.transpose(0, 1, 3, 2),
        input_imag.transpose(0, 1, 3, 2),
    )
    order = [
        2 * ((chip + chips - k) & (chips - 1)) + (core if same else 1 - core)
        for same in (True, False)
        for k in range(4)
    ]
    place = jnp.stack([lax.axis_index("z"), lax.axis_index("y"), *order]).astype(jnp.int32)
    summary, down_row = lax.optimization_barrier((summary, down_row))
    down_row = jnp.concatenate([down] + down_row, axis=0)
    down_all = lax.all_gather(down_row, "z", axis=0, tiled=False)
    row, group = pl.pallas_call(
        row_kernel,
        in_specs=[IN_SMEM] + [IN_VMEM] * 5,
        out_shape=[
            jax.ShapeDtypeStruct((4, *summary.shape), jnp.float32),
            jax.ShapeDtypeStruct(summary.shape, jnp.float32),
        ],
        name="row",
    )(place, summary, *(on_ring(summary, "y", k) for k in (1, -1, 2)), poles)
    found = [on_ring(group, "z", k) for k in range(1, 8)]
    found, own = lax.optimization_barrier((found, own))
    half = own.shape[0] // 2
    low, high = (own[:half], own[half:])
    low_left = on_ring(low, "y", 1)
    high_right = on_ring(high, "y", -1)
    high_left = on_ring(high, "y", 1)
    low_right = on_ring(low, "y", -1)
    mixed = pl.pallas_call(
        mixing_kernel,
        out_shape=jax.ShapeDtypeStruct((tokens, channels), jnp.bfloat16),
        in_specs=[IN_SMEM] + [IN_VMEM] * 17,
        scratch_shapes=[
            pltpu.VMEM((8, *summary.shape), jnp.float32),
            pltpu.VMEM((tokens, groups, lanes), jnp.float32),
            pltpu.VMEM((tokens, groups, lanes), jnp.float32),
            pltpu.VMEM((tokens, channels), jnp.float32),
            pltpu.VMEM((2 * channels, 2 * lanes), jnp.float32),
        ],
        name="mixing",
        cost_estimate=pl.CostEstimate(flops=COST, bytes_accessed=0, transcendentals=0),
    )(
        place,
        row,
        group,
        *found,
        mix_input,
        drive_real,
        drive_imag,
        decays,
        poles,
        output_real,
        output_imag,
        skip_gain[None],
    )
    product = jnp.dot(mixed, proj_weight, preferred_element_type=jnp.float32)
    branch = summed_over_tp(product[: tokens // 2], product[tokens // 2 :].astype(jnp.bfloat16))
    resid = stream.astype(jnp.float32) + branch
    scale = lax.rsqrt(jnp.mean(resid * resid, axis=-1, keepdims=True) + 1e-06)
    normed = (resid * scale * norm_gain).astype(jnp.bfloat16)
    normed, low_left, high_right = lax.optimization_barrier((normed, low_left, high_right))
    far = (on_ring(low_left, "y", 1), on_ring(high_right, "y", -1))
    mine = jnp.concatenate([normed] + [on_ring(normed, "x", k) for k in range(1, chips)], axis=0)
    rows = jnp.concatenate([mine, on_ring(mine, "c", 1)], axis=0)
    ffn = summed_over_tp(*feed_forward(
        place, rows, (own, low_left, high_left, low_right, high_right, *far, down_all)
    ))
    return (resid + 0.5 * ffn).astype(jnp.bfloat16)


def solution(mesh):
    torus = Mesh(mesh.devices.reshape(8, 4, 4, 2), ("z", "y", "x", "c"))
    everything = SP + TP
    in_specs = (
        P(SP, TP),
        P(everything, None),
        P(SP),
        P(TP),
        P(TP, None),
        P(TP, None),
        P(None, TP, None, None),
        P(None, TP, None, None),
        P(None, TP, None, None),
        P(None, TP, None, None),
        P(TP),
        P(TP, SP),
        P(TP, None),
        P(),
        P(SP, TP),
        P(SP, TP),
        P(TP, SP),
    )

    return jax.shard_map(
        local, mesh=torus, in_specs=in_specs, out_specs=P(everything, None), check_vma=False
    )
```

```python
import jax
import jax.numpy as jnp
from jax import lax
from jax.experimental import pallas as pl
from jax.experimental.pallas import tpu as pltpu
from jax.sharding import Mesh
from jax.sharding import PartitionSpec as P


GROUP = 16
FOLD = 16
COST = 2_000_000_000
SP = ("z", "y")
TP = ("x", "c")
HIGHEST = lax.Precision.HIGHEST


def discretize(log_dt, decay_rate, frequency):
    step_size = jnp.exp(log_dt)
    magnitude = jnp.exp(-step_size * decay_rate)
    angle_step = step_size * frequency
    state_real = magnitude * jnp.cos(angle_step)
    state_imag = magnitude * jnp.sin(angle_step)
    denominator = decay_rate * decay_rate + frequency * frequency
    shifted = state_real - 1.0
    zoh_real = (-shifted * decay_rate + state_imag * frequency) / denominator
    zoh_imag = (-state_imag * decay_rate - shifted * frequency) / denominator
    return (state_real, state_imag, zoh_real, zoh_imag)


def on_ring(array, axis, shift):
    size = lax.axis_size(axis)
    return lax.ppermute(array, axis, [(i, (i + shift) % size) for i in range(size)])


def flip_matrix(count, dtype):
    rows = lax.broadcasted_iota(jnp.int32, (count, count), 0)
    cols = lax.broadcasted_iota(jnp.int32, (count, count), 1)
    return jnp.where(rows + cols == count - 1, 1.0, 0.0).astype(dtype)


def times_transposed(left, right, precision=None):
    return lax.dot_general(
        left,
        right,
        (((1,), (1,)), ((), ())),
        precision=precision,
        preferred_element_type=jnp.float32,
    )


def side_by_side(left, right):
    return jnp.concatenate([left, right], axis=1)


def local_states_kernel(
    u_ref,
    keep_ref,
    docs_ref,
    dt_ref,
    rates_ref,
    freq_ref,
    map_real_ref,
    map_imag_ref,
    real_ref,
    imag_ref,
    decay_ref,
    pole_ref,
    summary_ref,
    drive_ref,
):
    tokens, channels = u_ref.shape
    groups, lanes = pole_ref.shape[1:]
    diagonal = lax.broadcasted_iota(jnp.int32, (groups, groups), 0) == lax.broadcasted_iota(
        jnp.int32, (groups, groups), 1
    )
    log_dt = jnp.sum(jnp.where(diagonal, dt_ref[...], 0.0), axis=1, keepdims=True)
    state_real, state_imag, zoh_real, zoh_imag = discretize(
        log_dt, side_by_side(rates_ref[...], rates_ref[...]), side_by_side(freq_ref[...], freq_ref[...])
    )
    pole_ref[0] = state_real
    pole_ref[1] = state_imag
    docs = docs_ref[...].astype(jnp.float32)
    place = lax.broadcasted_iota(jnp.int32, docs.shape, 1)
    from_left = (docs == pltpu.roll(docs, 1, 1)) | (place == 0)
    from_right = (docs == pltpu.roll(docs, tokens - 1, 1)) | (place == tokens - 1)
    keep = jnp.exp(keep_ref[...])
    factors = jnp.concatenate(
        [jnp.where(from_left, keep, 0.0), jnp.where(from_right, keep, 0.0)], axis=0
    )
    flip = flip_matrix(tokens, jnp.float32)
    rows = lax.broadcasted_iota(jnp.int32, (tokens, tokens), 0)
    cols = lax.broadcasted_iota(jnp.int32, (tokens, tokens), 1)
    same = jnp.where(rows == cols, 1.0, 0.0)
    ahead_factor = times_transposed(same, factors, HIGHEST)
    back_factor = times_transposed(flip, factors, HIGHEST)
    u = u_ref[...]
    backward = jnp.dot(
        flip.astype(jnp.bfloat16), u, preferred_element_type=jnp.float32
    ).astype(jnp.bfloat16)
    both = jnp.concatenate([u, backward], axis=1)
    ahead = lax.broadcasted_iota(jnp.int32, (tokens, lanes), 1) < lanes // 2
    part = ahead[:GROUP]
    drive_ref[...] = jnp.zeros(drive_ref.shape, jnp.float32)
    for g in range(groups):
        scale_real, scale_imag = (zoh_real[g : g + 1], zoh_imag[g : g + 1])
        in_real, in_imag = (
            side_by_side(ref[0, g], ref[1, g]) for ref in (map_real_ref, map_imag_ref)
        )
        map_real = scale_real * in_real - scale_imag * in_imag
        map_imag = scale_real * in_imag + scale_imag * in_real
        at = g * GROUP
        drive_ref[at : at + GROUP, :lanes] = jnp.where(part, map_real, 0.0)
        drive_ref[at : at + GROUP, lanes:] = jnp.where(part, map_imag, 0.0)
        drive_ref[channels + at : channels + at + GROUP, :lanes] = jnp.where(part, 0.0, map_real)
        drive_ref[channels + at : channels + at + GROUP, lanes:] = jnp.where(part, 0.0, map_imag)
        whole = drive_ref[...]
        drive_ref[at : at + GROUP] = jnp.zeros((GROUP, 2 * lanes), jnp.float32)
        drive_ref[channels + at : channels + at + GROUP] = jnp.zeros(
            (GROUP, 2 * lanes), jnp.float32
        )
        first = whole.astype(jnp.bfloat16)
        rest = whole - first.astype(jnp.float32)
        second = rest.astype(jnp.bfloat16)
        third = (rest - second.astype(jnp.float32)).astype(jnp.bfloat16)
        drive = jnp.dot(both, first, preferred_element_type=jnp.float32)
        drive = drive + jnp.dot(both, second, preferred_element_type=jnp.float32)
        drive = drive + jnp.dot(both, third, preferred_element_type=jnp.float32)
        real_ref[:, g, :] = drive[:, :lanes]
        imag_ref[:, g, :] = drive[:, lanes:]
        decay_ref[:, g, :] = jnp.where(
            ahead, ahead_factor[:, g : g + 1], back_factor[:, groups + g : groups + g + 1]
        )
    pole_real, pole_imag = (pole_ref[0], pole_ref[1])

    def step(t, carry):
        state_real, state_imag, product = carry
        factor = decay_ref[t]
        step_real, step_imag = (factor * pole_real, factor * pole_imag)
        return (
            step_real * state_real - step_imag * state_imag + real_ref[t],
            step_real * state_imag + step_imag * state_real + imag_ref[t],
            product * factor,
        )

    zero = jnp.zeros((groups, lanes), jnp.float32)
    state_real, state_imag, product = lax.fori_loop(
        0, tokens, step, (zero, zero, zero + 1.0), unroll=8
    )
    summary_ref[0] = state_real
    summary_ref[1] = state_imag
    summary_ref[2] = product
    first_doc, last_doc = (
        jnp.broadcast_to(docs[:, :1], (groups, lanes)),
        jnp.broadcast_to(docs[:, tokens - 1 :], (groups, lanes)),
    )
    summary_ref[3] = jnp.where(
        ahead[:groups], 8.0 * first_doc + last_doc, 8.0 * last_doc + first_doc
    )


def near_of(code):
    return jnp.floor(code * 0.125)


def squared(real, imag, times):
    for _ in range(times):
        real, imag = (real * real - imag * imag, 2.0 * real * imag)
    return (real, imag)


def pick(ref, ahead, j, last):
    return tuple(jnp.where(ahead, ref[j, k], ref[last - j, k]) for k in range(4))


def row_kernel(place_ref, own_ref, *refs):
    arrived, pole_ref, row_ref, group_ref = (refs[:3], refs[3], refs[4], refs[5])
    groups, lanes = pole_ref.shape[1:]
    row_ref[place_ref[1]] = own_ref[...]
    for back, ref in zip((1, 3, 2), arrived):
        row_ref[(place_ref[1] + 4 - back) % 4] = ref[...]
    ahead = lax.broadcasted_iota(jnp.int32, (groups, lanes), 1) < lanes // 2
    far_real, far_imag = squared(pole_ref[0], pole_ref[1], 8)
    state_real, state_imag, product, code = pick(row_ref, ahead, 0, 3)
    first = near_of(code)
    last = code - 8.0 * first
    for j in range(1, 4):
        local_real, local_imag, factor, code = pick(row_ref, ahead, j, 3)
        near = near_of(code)
        kept = jnp.where(near == last, factor, 0.0)
        last = code - 8.0 * near
        state_real, state_imag = (
            kept * (far_real * state_real - far_imag * state_imag) + local_real,
            kept * (far_real * state_imag + far_imag * state_real) + local_imag,
        )
        product = product * kept
    group_ref[0] = state_real
    group_ref[1] = state_imag
    group_ref[2] = product
    group_ref[3] = 8.0 * first + last


def mixing_kernel(
    place_ref,
    row_ref,
    *refs,
):
    group_refs = refs[:8]
    (
        u_ref,
        real_ref,
        imag_ref,
        decay_ref,
        pole_ref,
        read_real_ref,
        read_imag_ref,
        skip_ref,
        out_ref,
        all_ref,
        state_real_ref,
        state_imag_ref,
        mixed_ref,
        matrix_ref,
    ) = refs[8:]
    tokens, channels = u_ref.shape
    groups, lanes = pole_ref.shape[1:]
    pole_real, pole_imag = (pole_ref[0], pole_ref[1])
    for back, ref in enumerate(group_refs):
        all_ref[(place_ref[0] + 8 - back) % 8] = ref[...]
    ahead = lax.broadcasted_iota(jnp.int32, (groups, lanes), 1) < lanes // 2
    zero = jnp.zeros((groups, lanes), jnp.float32)
    state = (zero, zero, zero - 1.0)
    for ref, here, blocks, far in (
        (all_ref, place_ref[0], 8, squared(pole_real, pole_imag, 10)),
        (row_ref, place_ref[1], 4, squared(pole_real, pole_imag, 8)),
    ):
        for j in range(blocks - 1):
            state_real, state_imag, last = state
            local_real, local_imag, product, code = pick(ref, ahead, j, blocks - 1)
            ours = jnp.where(j < here, 1, 0)
            theirs = jnp.where(blocks - 1 - j > here, 1, 0)
            before = jnp.where(ahead, ours, theirs) > 0
            near = near_of(code)
            kept = jnp.where(near == last, product, 0.0)
            next_real = kept * (far[0] * state_real - far[1] * state_imag) + local_real
            next_imag = kept * (far[0] * state_imag + far[1] * state_real) + local_imag
            state = (
                jnp.where(before, next_real, state_real),
                jnp.where(before, next_imag, state_imag),
                jnp.where(before, code - 8.0 * near, last),
            )
    joined = near_of(row_ref[place_ref[1], 3]) == state[2]
    enter_real = jnp.where(joined, state[0], 0.0)
    enter_imag = jnp.where(joined, state[1], 0.0)

    def step(t, carry):
        state_real, state_imag = carry
        factor = decay_ref[t]
        step_real, step_imag = (factor * pole_real, factor * pole_imag)
        next_real = step_real * state_real - step_imag * state_imag + real_ref[t]
        next_imag = step_real * state_imag + step_imag * state_real + imag_ref[t]
        state_real_ref[t] = next_real
        state_imag_ref[t] = next_imag
        return (next_real, next_imag)

    lax.fori_loop(0, tokens, step, (enter_real, enter_imag), unroll=8)
    read = jnp.zeros((tokens, 2 * channels), jnp.float32)
    matrix_ref[...] = jnp.zeros(matrix_ref.shape, jnp.float32)
    part = lax.broadcasted_iota(jnp.int32, (GROUP, lanes), 1) < lanes // 2
    for g in range(groups):
        states = jnp.concatenate([state_real_ref[:, g, :], state_imag_ref[:, g, :]], axis=1)
        out_real = side_by_side(read_real_ref[0, g], read_real_ref[1, g])
        out_imag = -side_by_side(read_imag_ref[0, g], read_imag_ref[1, g])
        at = g * GROUP
        matrix_ref[at : at + GROUP, :lanes] = jnp.where(part, out_real, 0.0)
        matrix_ref[at : at + GROUP, lanes:] = jnp.where(part, out_imag, 0.0)
        matrix_ref[channels + at : channels + at + GROUP, :lanes] = jnp.where(part, 0.0, out_real)
        matrix_ref[channels + at : channels + at + GROUP, lanes:] = jnp.where(part, 0.0, out_imag)
        read = read + times_transposed(states, matrix_ref[...], HIGHEST)
        matrix_ref[at : at + GROUP] = jnp.zeros((GROUP, 2 * lanes), jnp.float32)
        matrix_ref[channels + at : channels + at + GROUP] = jnp.zeros(
            (GROUP, 2 * lanes), jnp.float32
        )
    backward = jnp.dot(
        flip_matrix(tokens, jnp.float32),
        read[:, channels:],
        precision=HIGHEST,
        preferred_element_type=jnp.float32,
    )
    pre = read[:, :channels] + backward + skip_ref[...] * u_ref[...].astype(jnp.float32)
    mixed_ref[...] = jax.nn.gelu(pre)
    rows = tokens // 8
    for k in range(8):
        start = pl.multiple_of(place_ref[2 + k] * rows, rows)
        out_ref[k * rows : (k + 1) * rows, :] = mixed_ref[pl.ds(start, rows), :].astype(
            jnp.bfloat16
        )


def silu_times(gate, up):
    return gate / (1.0 + jnp.exp(-gate)) * up


def feed_forward_kernel(
    place_ref,
    rows_ref,
    own_ref,
    low_left_ref,
    high_left_ref,
    low_right_ref,
    high_right_ref,
    low_far_ref,
    high_far_ref,
    down_ref,
    keep_ref,
    send_ref,
    gate_to,
    up_to,
    ends_to,
    down_to,
    sems,
):
    depth, hidden = down_to.shape[2:]
    half = low_far_ref.shape[0]
    column = [(place_ref[1] + 4 - back) % 4 for back in (0, 1, 3, 2)]
    copies = ([], [], [])
    low, high = (pl.ds(0, half), pl.ds(half, half))
    for source, zs, y in (
        (own_ref, pl.ds(0, 2 * half), column[0]),
        (low_left_ref, low, column[1]),
        (high_left_ref, high, column[1]),
        (low_right_ref, low, column[2]),
        (high_right_ref, high, column[2]),
        (low_far_ref, low, column[3]),
        (high_far_ref, high, column[3]),
    ):
        for which, target in enumerate((gate_to, up_to)):
            copies[which].append(
                pltpu.make_async_copy(
                    source.at[:, pl.ds(which * depth, depth)], target.at[zs, y], sems.at[which]
                )
            )
        for k in range(depth // FOLD):
            copies[1].append(
                pltpu.make_async_copy(
                    source.at[:, pl.ds(2 * depth, FOLD), pl.ds(128 * k, 128)],
                    ends_to.at[zs, y, pl.ds(FOLD * k, FOLD)],
                    sems.at[1],
                )
            )
    for m in range(4):
        copies[2].append(
            pltpu.make_async_copy(
                down_ref.at[:, pl.ds(m * depth, depth)], down_to.at[:, column[m]], sems.at[2]
            )
        )
    for group in copies:
        for copy in group:
            copy.start()
    rows = rows_ref[...]
    features = rows.shape[1]
    for copy in copies[0]:
        copy.wait()
    whole = gate_to.shape[3]
    gate = jnp.dot(
        rows, gate_to[...].reshape(features, whole), preferred_element_type=jnp.float32
    )
    for copy in copies[1]:
        copy.wait()
    up = jnp.dot(rows, up_to[...].reshape(features, whole), preferred_element_type=jnp.float32)
    ends = jnp.dot(rows, ends_to[...].reshape(features, 128), preferred_element_type=jnp.float32)
    first = lax.broadcasted_iota(jnp.int32, ends.shape, 1) < 64
    last = jnp.where(first, silu_times(ends, pltpu.roll(ends, 64, 1)), 0.0)
    inner = jnp.concatenate([silu_times(gate, up), last], axis=1).astype(jnp.bfloat16)
    for copy in copies[2]:
        copy.wait()
    near = keep_ref.shape[0]
    count = 2
    width = count * 4 * depth
    for z in range(0, down_to.shape[0], count):
        made = times_transposed(inner, down_to[z : z + count].reshape(width, hidden))
        at = z * 4 * depth
        keep_ref[:, at : at + width] = made[:near]
        send_ref[:, at : at + width] = made[near:].astype(jnp.bfloat16)


def feed_forward(place, rows, pieces):
    tokens, features = rows.shape
    widths = (pieces[0].shape[2], pieces[0].shape[2], 128, pieces[-1].shape[2])
    return pl.pallas_call(
        feed_forward_kernel,
        in_specs=[IN_SMEM, IN_VMEM] + [pl.BlockSpec(memory_space=pl.ANY)] * len(pieces),
        out_shape=[
            jax.ShapeDtypeStruct((tokens // 2, features), jnp.float32),
            jax.ShapeDtypeStruct((tokens // 2, features), jnp.bfloat16),
        ],
        scratch_shapes=[
            pltpu.VMEM((8, 4, features // 32, width), jnp.bfloat16) for width in widths
        ]
        + [pltpu.SemaphoreType.DMA((3,))],
        name="feed_forward",
    )(place, rows, *pieces)


IN_VMEM = pl.BlockSpec(memory_space=pltpu.VMEM)
IN_SMEM = pl.BlockSpec(memory_space=pltpu.SMEM)


def pack_kernel(gate_ref, up_ref, out_ref):
    depth = gate_ref.shape[0]
    whole = out_ref.shape[1]
    out_ref[:depth] = gate_ref[:, :whole]
    out_ref[depth : 2 * depth] = up_ref[:, :whole]
    ends = side_by_side(gate_ref[:, whole:], up_ref[:, whole:])
    for k in range(depth // FOLD):
        out_ref[2 * depth :, 128 * k : 128 * (k + 1)] = ends[FOLD * k : FOLD * (k + 1)]
    used = 128 * (depth // FOLD)
    out_ref[2 * depth :, used:] = jnp.zeros((FOLD, whole - used), out_ref.dtype)


def packed(gate, up):
    depth, hidden = gate.shape
    return pl.pallas_call(
        pack_kernel,
        out_shape=jax.ShapeDtypeStruct((2 * depth + FOLD, hidden // 128 * 128), gate.dtype),
        name="pack",
    )(gate, up)


def halves_kernel(whole_ref, low_ref, high_ref, buffer_ref, in_sems, out_sems):
    half = low_ref.shape[0]
    order = [at + k for k in range(half) for at in (0, half)]
    arriving = {
        k: pltpu.make_async_copy(whole_ref.at[k], buffer_ref.at[k], in_sems.at[k]) for k in order
    }
    leaving = {
        k: pltpu.make_async_copy(
            buffer_ref.at[k], (low_ref if k < half else high_ref).at[k % half], out_sems.at[k]
        )
        for k in order
    }
    for k in order:
        arriving[k].start()
    for k in order:
        arriving[k].wait()
        leaving[k].start()
    for k in order:
        leaving[k].wait()


def with_other_core(keep, send):
    return keep + on_ring(send, "c", 1).astype(jnp.float32)


def over_chips(pair):
    chips = lax.axis_size("x")
    rows = pair.shape[0] // chips
    total = pair[:rows]
    away = pair.astype(jnp.bfloat16)
    for k in range(1, chips):
        arrived = on_ring(away[k * rows : (k + 1) * rows], "x", -k)
        total = total + arrived.astype(jnp.float32)
    return total


def local(
    mix_input,
    stream,
    doc_ids,
    log_dt,
    decay_rate,
    frequency,
    input_real,
    input_imag,
    output_real,
    output_imag,
    skip_gain,
    log_keep,
    proj_weight,
    norm_gain,
    gate_weight,
    up_weight,
    down_weight,
):
    chips = lax.axis_size("x")
    chip, core = (lax.axis_index("x"), lax.axis_index("c"))
    tokens, channels = mix_input.shape
    groups, states = decay_rate.shape
    lanes = 2 * states
    spare = -gate_weight.shape[1] % 128
    gate_up = packed(gate_weight, up_weight)
    own = lax.all_gather(gate_up, "z", axis=0, tiled=False)
    down = jnp.pad(down_weight.T, ((0, 0), (0, spare)))
    down_row = [on_ring(down, "y", k) for k in (1, -1, 2)]
    by_token = jax.ShapeDtypeStruct((tokens, groups, lanes), jnp.float32)
    drive_real, drive_imag, decays, poles, summary = pl.pallas_call(
        local_states_kernel,
        out_shape=[by_token] * 3
        + [jax.ShapeDtypeStruct((k, groups, lanes), jnp.float32) for k in (2, 4)],
        scratch_shapes=[pltpu.VMEM((2 * channels, 2 * lanes), jnp.float32)],
        name="local_states",
    )(
        mix_input,
        log_keep,
        doc_ids[None],
        log_dt[None],
        decay_rate,
        frequency,
        input_real.transpose(0, 1, 3, 2),
        input_imag.transpose(0, 1, 3, 2),
    )
    order = [
        2 * ((chip + chips - k) & (chips - 1)) + (core if same else 1 - core)
        for same in (True, False)
        for k in range(4)
    ]
    place = jnp.stack([lax.axis_index("z"), lax.axis_index("y"), *order]).astype(jnp.int32)
    summary, down_row = lax.optimization_barrier((summary, down_row))
    down_row = jnp.concatenate([down] + down_row, axis=0)
    down_all = lax.all_gather(down_row, "z", axis=0, tiled=False)
    row, group = pl.pallas_call(
        row_kernel,
        in_specs=[IN_SMEM] + [IN_VMEM] * 5,
        out_shape=[
            jax.ShapeDtypeStruct((4, *summary.shape), jnp.float32),
            jax.ShapeDtypeStruct(summary.shape, jnp.float32),
        ],
        name="row",
    )(place, summary, *(on_ring(summary, "y", k) for k in (1, -1, 2)), poles)
    found = [on_ring(group, "z", k) for k in range(1, 8)]
    half = own.shape[0] // 2
    anywhere = pl.BlockSpec(memory_space=pl.ANY)
    low, high = pl.pallas_call(
        halves_kernel,
        in_specs=[anywhere],
        out_specs=[anywhere] * 2,
        out_shape=[jax.ShapeDtypeStruct((half, *own.shape[1:]), own.dtype)] * 2,
        scratch_shapes=[pltpu.VMEM(own.shape, own.dtype)]
        + [pltpu.SemaphoreType.DMA((2 * half,))] * 2,
        name="halves",
    )(own)
    low_left = on_ring(low, "y", 1)
    high_right = on_ring(high, "y", -1)
    high_left = on_ring(high, "y", 1)
    low_right = on_ring(low, "y", -1)
    mixed = pl.pallas_call(
        mixing_kernel,
        out_shape=jax.ShapeDtypeStruct((tokens, channels), jnp.bfloat16),
        in_specs=[IN_SMEM] + [IN_VMEM] * 17,
        scratch_shapes=[
            pltpu.VMEM((8, *summary.shape), jnp.float32),
            pltpu.VMEM((tokens, groups, lanes), jnp.float32),
            pltpu.VMEM((tokens, groups, lanes), jnp.float32),
            pltpu.VMEM((tokens, channels), jnp.float32),
            pltpu.VMEM((2 * channels, 2 * lanes), jnp.float32),
        ],
        name="mixing",
        cost_estimate=pl.CostEstimate(flops=COST, bytes_accessed=0, transcendentals=0),
    )(
        place,
        row,
        group,
        *found,
        mix_input,
        drive_real,
        drive_imag,
        decays,
        poles,
        output_real,
        output_imag,
        skip_gain[None],
    )
    product = jnp.dot(mixed, proj_weight, preferred_element_type=jnp.float32)
    pair = with_other_core(product[: tokens // 2], product[tokens // 2 :].astype(jnp.bfloat16))
    branch = over_chips(pair)
    branch, low_left, high_right = lax.optimization_barrier((branch, low_left, high_right))
    far = (on_ring(low_left, "y", 1), on_ring(high_right, "y", -1))
    resid = stream.astype(jnp.float32) + branch
    scale = lax.rsqrt(jnp.mean(resid * resid, axis=-1, keepdims=True) + 1e-06)
    normed = (resid * scale * norm_gain).astype(jnp.bfloat16)
    arrived = [on_ring(normed, "x", k) for k in range(1, chips)]
    mine = jnp.concatenate([normed] + arrived, axis=0)
    rows = jnp.concatenate([mine, on_ring(mine, "c", 1)], axis=0)
    pieces = (own, low_left, high_left, low_right, high_right, *far, down_all)
    ffn = over_chips(with_other_core(*feed_forward(place, rows, pieces)))
    return (resid + 0.5 * ffn).astype(jnp.bfloat16)


def solution(mesh):
    torus = Mesh(mesh.devices.reshape(8, 4, 4, 2), ("z", "y", "x", "c"))
    everything = SP + TP
    in_specs = (
        P(SP, TP),
        P(everything, None),
        P(SP),
        P(TP),
        P(TP, None),
        P(TP, None),
        P(None, TP, None, None),
        P(None, TP, None, None),
        P(None, TP, None, None),
        P(None, TP, None, None),
        P(TP),
        P(TP, SP),
        P(TP, None),
        P(),
        P(SP, TP),
        P(SP, TP),
        P(TP, SP),
    )

    return jax.shard_map(
        local, mesh=torus, in_specs=in_specs, out_specs=P(everything, None), check_vma=False
    )
```
